32 devices in a mesh: grp: 2 (over y), sp: 4 (over z), tp: 4 (over x, core).
Axes of the slice: x: 2, y: 2, z: 4, core: 2. Of those that a mesh axis runs over, the one named last changes fastest.
Arguments:
- resid: bfloat16 [5120, 2048], P(('grp', 'sp'), 'tp'), parts along dimension 0, may hold values from -6 to 6
- queries: bfloat16 [5120, 2048], P(('grp', 'sp'), 'tp'), parts along dimension 0, may hold values from -150 to 150
- keys_values: bfloat16 [5120, 8, 128], P(('grp', 'sp'), 'tp'), parts along dimension 0, may hold values from -4.5 to 4.5
- sink: float32 [32], P('tp'), may hold values from 3 to 7
- out_weight: bfloat16 [2048, 2048], P('tp'), may hold values from -2.390625 to 2.390625
- norm_gain: float32 [2048], replicated, may hold values from 0.1 to 1.9
- gate_weight: bfloat16 [2048, 5632], P('sp', 'tp'), may hold values from -0.125 to 0.125
- up_weight: bfloat16 [2048, 5632], P('sp', 'tp'), may hold values from -0.125 to 0.125
- down_weight: bfloat16 [5632, 2048], P('tp', 'sp'), may hold values from -0.078125 to 0.078125
Outputs:
- mixed: bfloat16 [5120, 2048], P(('grp', 'sp'), 'tp'), parts along dimension 0
The draws below stay inside these ranges and needn't reach their ends.
There are 2 independent parts, one for each index of `grp`. The reference program is written for one: setup_inputs(seed, part) draws one part's arguments, and reference() takes and returns one part's arrays. A program takes and returns all parts, laid end to end along the dimension named above; an argument that names none is the same for every part. Nothing has to cross between parts.
All inputs are finite; a program needn't handle non-finite values.
Results may differ from the reference program's by a relative error of at most 0.008.
Values may be sent and summed in bfloat16 or wider, within the bound.
A program may use at most 128 MiB of HBM per device.

```python
import jax
import jax.numpy as jnp
from jax import lax

D = 2048
HEADS = 32
KV_HEADS = 8
HEAD_DIM = 64
FF = 5632
WINDOW = 128
GRID_W = 64
TOKENS = 2560


def joint_draw(key):
    both = jnp.clip(jax.random.normal(jax.random.fold_in(key, 11), (TOKENS, KV_HEADS, 2 * HEAD_DIM), jnp.float32), -4.5, 4.5)
    drawn = jnp.clip(jax.random.normal(jax.random.fold_in(key, 12), (TOKENS, HEADS * HEAD_DIM), jnp.float32), -4.5, 4.5)
    return (drawn, both)


def draw_queries(key, part):
    drawn, both = joint_draw(key)
    return drawn.astype(jnp.bfloat16)


def draw_keys_values(key, part):
    drawn, both = joint_draw(key)
    return both.astype(jnp.bfloat16)


def shard_levels(rng, extent, split, smallest, largest):
    gain, own = 1.0, jax.random.fold_in(rng, 6)
    for dim, blocks in split:
        steps = jnp.exp(jax.random.uniform(jax.random.fold_in(own, dim), (blocks,), jnp.float32, smallest / len(split), largest / len(split)))
        gain = gain * jnp.repeat(steps, extent[dim] // blocks).reshape([-1 if axis == dim else 1 for axis in range(len(extent))])
    return gain


def normal_values(key, dims, deviation, most, split=(), held_as=jnp.bfloat16):
    entries = jax.random.normal(key, dims, jnp.float32) * deviation
    if len(split) > 0:
        entries = shard_levels(key, dims, split, -0.22, 0.18) * entries
    return jnp.clip(entries, min=-most, max=most).astype(held_as)


def setup_inputs(seed: int = 0, part: int = 0) -> dict:
    streams_of = jax.random.split(jax.random.key(seed), 10)
    part_keys = jax.random.split(jax.random.fold_in(streams_of[9], part), 10)
    return {
        "resid": normal_values(part_keys[0], (TOKENS, D), 1.0, 6.0, ((0, 4), (1, 4))),
        "queries": draw_queries(jax.random.fold_in(jax.random.fold_in(streams_of[9], part), 71), part),
        "keys_values": draw_keys_values(jax.random.fold_in(jax.random.fold_in(streams_of[9], part), 71), part),
        "sink": jnp.clip(3.0 + 4.0 * jax.random.uniform(streams_of[3], (HEADS,), jnp.float32) ** shard_levels(streams_of[3], (HEADS,), ((0, 4),), -0.2, 0.2), 3.0, 7.0),
        "out_weight": normal_values(streams_of[4], (HEADS * HEAD_DIM, D), 0.4, 2.390625, ((0, 4),)),
        "norm_gain": jnp.clip(1.0 + 0.18 * jax.random.normal(streams_of[5], (D,), jnp.float32), 0.1, 1.9),
        "gate_weight": normal_values(streams_of[6], (D, FF), D ** -0.5, 0.125, ((0, 4), (1, 4))),
        "up_weight": normal_values(streams_of[7], (D, FF), D ** -0.5, 0.125, ((0, 4), (1, 4))),
        "down_weight": normal_values(streams_of[8], (FF, D), FF ** -0.5, 0.078125, ((0, 4), (1, 4))),
    }


def rotate(values, positions):
    quarter = 16
    inverse = 10000.0 ** (-jnp.arange(quarter, dtype=jnp.float32) / quarter)

    def turn(part, place):
        angle = place.astype(jnp.float32)[:, None] * inverse[None, :]
        cosine = jnp.cos(angle)[:, None, :]
        sine = jnp.sin(angle)[:, None, :]
        first, second = (part[..., :quarter], part[..., quarter:])
        return jnp.concatenate([first * cosine - second * sine, second * cosine + first * sine], axis=-1)
    grid_row = positions // GRID_W
    grid_col = positions % GRID_W
    return jnp.concatenate([turn(values[..., :32], grid_row), turn(values[..., 32:], grid_col)], axis=-1)

def reference(resid, queries, keys_values, sink, out_weight, norm_gain, gate_weight, up_weight, down_weight):
    group = HEADS // KV_HEADS
    positions = jnp.arange(TOKENS, dtype=jnp.int32)
    rotated_q = rotate(queries.astype(jnp.float32).reshape(TOKENS, HEADS, HEAD_DIM), positions).astype(jnp.bfloat16)
    rotated_k = rotate(keys_values[..., :HEAD_DIM].astype(jnp.float32), positions).astype(jnp.bfloat16)
    padded_k = jnp.pad(rotated_k, ((WINDOW, WINDOW), (0, 0), (0, 0)))
    padded_v = jnp.pad(keys_values[..., HEAD_DIM:], ((WINDOW, WINDOW), (0, 0), (0, 0)))
    sink_grid = sink.reshape(KV_HEADS, group)[:, :, None]

    def block(index):
        start = (index * WINDOW).astype(jnp.int32)
        zero = jnp.int32(0)
        query_block = lax.dynamic_slice(rotated_q, (start, zero, zero), (WINDOW, HEADS, HEAD_DIM))
        key_block = lax.dynamic_slice(padded_k, (start, zero, zero), (3 * WINDOW, KV_HEADS, HEAD_DIM))
        value_block = lax.dynamic_slice(padded_v, (start, zero, zero), (3 * WINDOW, KV_HEADS, HEAD_DIM))
        grouped = query_block.astype(jnp.float32).reshape(WINDOW, KV_HEADS, group, HEAD_DIM)
        scores = jnp.einsum('qkgd,jkd->kgqj', grouped, key_block.astype(jnp.float32)) * HEAD_DIM ** (-0.5)
        query_pos = start + jnp.arange(WINDOW, dtype=jnp.int32)
        key_pos = start - WINDOW + jnp.arange(3 * WINDOW, dtype=jnp.int32)
        valid = (jnp.abs(query_pos[:, None] - key_pos[None, :]) <= WINDOW) & (key_pos[None, :] >= 0) & (key_pos[None, :] < TOKENS)
        scores = jnp.where(valid[None, None], scores, jnp.float32(-1e+30))
        top = jnp.maximum(lax.optimization_barrier(jnp.max(scores, axis=-1)), sink_grid)
        expo = jnp.exp(scores - top[..., None])
        total = lax.optimization_barrier(jnp.sum(expo, axis=-1)) + jnp.exp(sink_grid - top)
        probs = (expo / total[..., None]).astype(jnp.bfloat16)
        result = jnp.einsum('kgqj,jkd->qkgd', probs.astype(jnp.float32), value_block.astype(jnp.float32))
        return result.astype(jnp.bfloat16).reshape(WINDOW, HEADS * HEAD_DIM)
    attended = lax.map(block, jnp.arange(TOKENS // WINDOW, dtype=jnp.int32)).reshape(TOKENS, HEADS * HEAD_DIM)
    stream = (resid.astype(jnp.float32) + jnp.dot(attended, out_weight, preferred_element_type=jnp.float32)).astype(jnp.bfloat16)
    widened = stream.astype(jnp.float32)
    normed = (widened * lax.rsqrt(lax.optimization_barrier(jnp.mean(widened * widened, axis=-1, keepdims=True)) + 1e-06) * norm_gain).astype(jnp.bfloat16)
    gate = jnp.dot(normed, gate_weight, preferred_element_type=jnp.float32)
    up = jnp.dot(normed, up_weight, preferred_element_type=jnp.float32)
    hidden = (jax.nn.silu(gate) * up).astype(jnp.bfloat16)
    return (stream.astype(jnp.float32) + jnp.dot(hidden, down_weight, preferred_element_type=jnp.float32)).astype(jnp.bfloat16)
```

```python
import jax
import jax.numpy as jnp
from jax import lax
from jax.sharding import PartitionSpec as P

HEAD_DIM = 64
WINDOW = 128
GRID_W = 64


def with_halo(cells, sides, width):
    for axis, dim in sides:
        count = lax.axis_size(axis)
        ends = count - 1
        head = lax.slice_in_dim(cells, 0, width, axis=dim)
        tail = lax.slice_in_dim(cells, cells.shape[dim] - width, cells.shape[dim], axis=dim)
        cells = jnp.concatenate(
            [
                lax.ppermute(tail, axis, [(i, (i + 1) % count) for i in range(ends)]),
                cells,
                lax.ppermute(head, axis, [((i + 1) % count, i) for i in range(ends)]),
            ],
            axis=dim,
        )
    return cells


def rotate(values, positions):
    quarter = 16
    inverse = 10000.0 ** (-jnp.arange(quarter, dtype=jnp.float32) / quarter)

    def turn(part, place):
        angle = place.astype(jnp.float32)[:, None] * inverse[None, :]
        cosine = jnp.cos(angle)[:, None, :]
        sine = jnp.sin(angle)[:, None, :]
        first, second = (part[..., :quarter], part[..., quarter:])
        return jnp.concatenate(
            [first * cosine - second * sine, second * cosine + first * sine], axis=-1
        )

    grid_row = positions // GRID_W
    grid_col = positions % GRID_W
    return jnp.concatenate(
        [turn(values[..., :32], grid_row), turn(values[..., 32:], grid_col)], axis=-1
    )


def share(weight, axis):
    parts = lax.axis_size("grp")
    size = weight.shape[axis] // parts
    part = lax.dynamic_slice_in_dim(weight, lax.axis_index("grp") * size, size, axis)
    return lax.all_gather(part, ("sp", "grp"), axis=axis, tiled=True)


def body(
    resid, queries, keys_values, sink, out_weight, norm_gain, gate_weight, up_weight, down_weight
):
    tok = queries.shape[0]
    heads_here = queries.shape[1] // HEAD_DIM
    kv_here = keys_values.shape[1]
    group = heads_here // kv_here
    cols = resid.shape[1]
    offset = lax.axis_index("sp") * tok
    total_tokens = tok * lax.axis_size("sp")
    positions = offset + jnp.arange(tok, dtype=jnp.int32)
    rotated_q = rotate(
        queries.astype(jnp.float32).reshape(tok, heads_here, HEAD_DIM), positions
    ).astype(jnp.bfloat16)
    rotated_k = rotate(keys_values[..., :HEAD_DIM].astype(jnp.float32), positions).astype(
        jnp.bfloat16
    )
    joined = jnp.concatenate([rotated_k, keys_values[..., HEAD_DIM:]], axis=-1)
    padded = with_halo(joined, (("sp", 0),), WINDOW)
    blocks = tok // WINDOW
    key_blocks = jnp.stack(
        [padded[index * WINDOW : index * WINDOW + 3 * WINDOW] for index in range(blocks)]
    )
    grouped = rotated_q.reshape(blocks, WINDOW, kv_here, group, HEAD_DIM)
    scores = jnp.einsum(
        "nqkgd,njkd->nkgqj", grouped, key_blocks[..., :HEAD_DIM], preferred_element_type=jnp.float32
    ) * HEAD_DIM ** (-0.5)
    block_start = offset + WINDOW * jnp.arange(blocks, dtype=jnp.int32)
    query_pos = block_start[:, None] + jnp.arange(WINDOW, dtype=jnp.int32)[None, :]
    key_pos = block_start[:, None] - WINDOW + jnp.arange(3 * WINDOW, dtype=jnp.int32)[None, :]
    valid = (
        (jnp.abs(query_pos[:, :, None] - key_pos[:, None, :]) <= WINDOW)
        & (key_pos[:, None, :] >= 0)
        & (key_pos[:, None, :] < total_tokens)
    )
    scores = jnp.where(valid[:, None, None], scores, jnp.float32(-1e30))
    sink_grid = sink.reshape(kv_here, group)[None, :, :, None]
    top = jnp.maximum(jnp.max(scores, axis=-1), sink_grid)
    expo = jnp.exp(scores - top[..., None])
    denom = jnp.sum(expo, axis=-1) + jnp.exp(sink_grid - top)
    probs = (expo / denom[..., None]).astype(jnp.bfloat16)
    attended = jnp.einsum(
        "nkgqj,njkd->nqkgd", probs, key_blocks[..., HEAD_DIM:], preferred_element_type=jnp.float32
    )
    attended = attended.astype(jnp.bfloat16).reshape(tok, heads_here * HEAD_DIM)
    attn_rows, resid_rows = (
        lax.all_to_all(attended, "tp", split_axis=0, concat_axis=1, tiled=True),
        lax.all_to_all(resid, "tp", split_axis=0, concat_axis=1, tiled=True),
    )
    whole_out = lax.all_gather(out_weight, "tp", axis=0, tiled=True)
    stream_part = (
        resid_rows.astype(jnp.float32)
        + jnp.dot(attn_rows, whole_out, preferred_element_type=jnp.float32)
    ).astype(jnp.bfloat16)
    stream = lax.all_gather(stream_part, "tp", axis=0, tiled=True)
    stream_cols = lax.dynamic_slice_in_dim(stream, lax.axis_index("tp") * cols, cols, 1)
    widened = stream.astype(jnp.float32)
    normed = (
        widened * lax.rsqrt(jnp.mean(widened * widened, axis=-1, keepdims=True) + 1e-06) * norm_gain
    ).astype(jnp.bfloat16)
    gate = jnp.dot(
        normed,
        share(gate_weight, 0),
        preferred_element_type=jnp.float32,
    )
    up = jnp.dot(
        normed,
        share(up_weight, 0),
        preferred_element_type=jnp.float32,
    )
    hidden = (jax.nn.silu(gate) * up).astype(jnp.bfloat16)
    terms = jnp.dot(
        hidden,
        share(down_weight, 1),
        preferred_element_type=jnp.float32,
    )
    summed = lax.psum_scatter(
        terms.astype(jnp.bfloat16), "tp", scatter_dimension=1, tiled=True
    ).astype(jnp.float32)
    return (stream_cols.astype(jnp.float32) + summed).astype(jnp.bfloat16)


def solution(mesh):
    return jax.shard_map(
        body,
        mesh=mesh,
        in_specs=(
            P(("grp", "sp"), "tp"),
            P(("grp", "sp"), "tp"),
            P(("grp", "sp"), "tp", None),
            P("tp"),
            P("tp", None),
            P(),
            P("sp", "tp"),
            P("sp", "tp"),
            P("tp", "sp"),
        ),
        out_specs=P(("grp", "sp"), "tp"),
        check_vma=False,
    )
```

```python
import jax
import jax.numpy as jnp
from jax import lax
from jax.sharding import PartitionSpec as P

HEAD_DIM = 64
WINDOW = 128
GRID_W = 64


def with_halo(cells, sides, width):
    for axis, dim in sides:
        count = lax.axis_size(axis)
        ends = count - 1
        head = lax.slice_in_dim(cells, 0, width, axis=dim)
        tail = lax.slice_in_dim(cells, cells.shape[dim] - width, cells.shape[dim], axis=dim)
        cells = jnp.concatenate(
            [
                lax.ppermute(tail, axis, [(i, (i + 1) % count) for i in range(ends)]),
                cells,
                lax.ppermute(head, axis, [((i + 1) % count, i) for i in range(ends)]),
            ],
            axis=dim,
        )
    return cells


def rotate(values, positions):
    quarter = 16
    inverse = 10000.0 ** (-jnp.arange(quarter, dtype=jnp.float32) / quarter)

    def turn(part, place):
        angle = place.astype(jnp.float32)[:, None] * inverse[None, :]
        cosine = jnp.cos(angle)[:, None, :]
        sine = jnp.sin(angle)[:, None, :]
        first, second = (part[..., :quarter], part[..., quarter:])
        return jnp.concatenate(
            [first * cosine - second * sine, second * cosine + first * sine], axis=-1
        )

    grid_row = positions // GRID_W
    grid_col = positions % GRID_W
    return jnp.concatenate(
        [turn(values[..., :32], grid_row), turn(values[..., 32:], grid_col)], axis=-1
    )


def share(weight, axis):
    parts = lax.axis_size("grp")
    size = weight.shape[axis] // parts
    part = lax.dynamic_slice_in_dim(weight, lax.axis_index("grp") * size, size, axis)
    return lax.all_gather(part, ("sp", "grp"), axis=axis, tiled=True)


def relay(blocks, axes):
    count, parts = lax.axis_size("sp"), lax.axis_size("grp")
    here, group = lax.axis_index("sp"), lax.axis_index("grp")

    def place(whole, value, axis, block, source, part):
        rows = block.shape[0]
        start = part * (rows // parts)
        at = (source * rows + start, 0) if axis == 0 else (start, source * block.shape[1])
        return lax.dynamic_update_slice(whole, value, at)

    wholes, right, left = [], [], []
    for block, axis in zip(blocks, axes):
        shape = list(block.shape)
        shape[axis] *= count
        wholes.append(place(jnp.zeros(shape, block.dtype), block, axis, block, here, 0))
        rows = block.shape[0] // parts
        part = lax.dynamic_slice_in_dim(block, group * rows, rows, 0)
        right.append([part])
        left.append([part])
    for step in range(1, count):
        source = jnp.where(here >= step, here - step, step)
        for index, (block, axis) in enumerate(zip(blocks, axes)):
            right[index].append(
                lax.ppermute(
                    right[index][-1], "sp", [(i, i + 1) for i in range(step - 1, count - 1)]
                )
            )
            left[index].append(
                lax.ppermute(left[index][-1], "sp", [(i + 1, i) for i in range(count - step)])
            )
            came = [left[index][step - i] for i in range(step)] + [right[index][step]]
            value = lax.select_n(jnp.minimum(here, step), *came)
            whole = place(wholes[index], value, axis, block, source, group)
            for shift in range(1, parts):
                other = lax.ppermute(value, "grp", [(i, (i + shift) % parts) for i in range(parts)])
                whole = place(whole, other, axis, block, source, (group - shift) % parts)
            wholes[index] = whole
    return wholes


def body(
    resid, queries, keys_values, sink, out_weight, norm_gain, gate_weight, up_weight, down_weight
):
    tok = queries.shape[0]
    heads_here = queries.shape[1] // HEAD_DIM
    kv_here = keys_values.shape[1]
    group = heads_here // kv_here
    cols = resid.shape[1]
    offset = lax.axis_index("sp") * tok
    total_tokens = tok * lax.axis_size("sp")
    positions = offset + jnp.arange(tok, dtype=jnp.int32)
    rotated_q = rotate(
        queries.astype(jnp.float32).reshape(tok, heads_here, HEAD_DIM), positions
    ).astype(jnp.bfloat16)
    padded = with_halo(keys_values, (("sp", 0),), WINDOW)
    if lax.axis_size("sp") <= 8:
        padded, gate_weight, up_weight, down_weight = lax.optimization_barrier(
            (padded, gate_weight, up_weight, down_weight)
        )
        both = jnp.concatenate([gate_weight, up_weight], axis=1)
        whole_both, whole_down = relay((both, down_weight), (0, 1))
    else:
        whole_both = jnp.concatenate([share(gate_weight, 0), share(up_weight, 0)], axis=1)
        whole_down = share(down_weight, 1)
    key_positions = offset - WINDOW + jnp.arange(tok + 2 * WINDOW, dtype=jnp.int32)
    rotated_k = rotate(padded[..., :HEAD_DIM].astype(jnp.float32), key_positions).astype(
        jnp.bfloat16
    )
    padded = jnp.concatenate([rotated_k, padded[..., HEAD_DIM:]], axis=-1)
    blocks = tok // WINDOW
    key_blocks = jnp.stack(
        [padded[index * WINDOW : index * WINDOW + 3 * WINDOW] for index in range(blocks)]
    )
    grouped = rotated_q.reshape(blocks, WINDOW, kv_here, group, HEAD_DIM)
    scores = jnp.einsum(
        "nqkgd,njkd->nkgqj", grouped, key_blocks[..., :HEAD_DIM], preferred_element_type=jnp.float32
    ) * HEAD_DIM ** (-0.5)
    block_start = offset + WINDOW * jnp.arange(blocks, dtype=jnp.int32)
    query_pos = block_start[:, None] + jnp.arange(WINDOW, dtype=jnp.int32)[None, :]
    key_pos = block_start[:, None] - WINDOW + jnp.arange(3 * WINDOW, dtype=jnp.int32)[None, :]
    valid = (
        (jnp.abs(query_pos[:, :, None] - key_pos[:, None, :]) <= WINDOW)
        & (key_pos[:, None, :] >= 0)
        & (key_pos[:, None, :] < total_tokens)
    )
    scores = jnp.where(valid[:, None, None], scores, jnp.float32(-1e30))
    sink_grid = sink.reshape(kv_here, group)[None, :, :, None]
    top = jnp.maximum(jnp.max(scores, axis=-1), sink_grid)
    expo = jnp.exp(scores - top[..., None])
    denom = jnp.sum(expo, axis=-1) + jnp.exp(sink_grid - top)
    probs = (expo / denom[..., None]).astype(jnp.bfloat16)
    attended = jnp.einsum(
        "nkgqj,njkd->nqkgd", probs, key_blocks[..., HEAD_DIM:], preferred_element_type=jnp.float32
    )
    attended = attended.astype(jnp.bfloat16).reshape(tok, heads_here * HEAD_DIM)
    attn_rows, resid_rows = (
        lax.all_to_all(attended, "tp", split_axis=0, concat_axis=1, tiled=True),
        lax.all_to_all(resid, "tp", split_axis=0, concat_axis=1, tiled=True),
    )
    whole_out = lax.all_gather(out_weight, "tp", axis=0, tiled=True)
    stream_part = (
        resid_rows.astype(jnp.float32)
        + jnp.dot(attn_rows, whole_out, preferred_element_type=jnp.float32)
    ).astype(jnp.bfloat16)
    stream = lax.all_gather(stream_part, "tp", axis=0, tiled=True)
    stream_cols = lax.dynamic_slice_in_dim(stream, lax.axis_index("tp") * cols, cols, 1)
    widened = stream.astype(jnp.float32)
    normed = (
        widened * lax.rsqrt(jnp.mean(widened * widened, axis=-1, keepdims=True) + 1e-06) * norm_gain
    ).astype(jnp.bfloat16)
    gate_up = jnp.dot(normed, whole_both, preferred_element_type=jnp.float32)
    gate, up = jnp.split(gate_up, 2, axis=1)
    hidden = (jax.nn.silu(gate) * up).astype(jnp.bfloat16)
    terms = jnp.dot(
        hidden,
        whole_down,
        preferred_element_type=jnp.float32,
    )
    summed = lax.psum_scatter(
        terms.astype(jnp.bfloat16), "tp", scatter_dimension=1, tiled=True
    ).astype(jnp.float32)
    return (stream_cols.astype(jnp.float32) + summed).astype(jnp.bfloat16)


def solution(mesh):
    return jax.shard_map(
        body,
        mesh=mesh,
        in_specs=(
            P(("grp", "sp"), "tp"),
            P(("grp", "sp"), "tp"),
            P(("grp", "sp"), "tp", None),
            P("tp"),
            P("tp", None),
            P(),
            P("sp", "tp"),
            P("sp", "tp"),
            P("tp", "sp"),
        ),
        out_specs=P(("grp", "sp"), "tp"),
        check_vma=False,
    )
```

```python
import jax
import jax.numpy as jnp
from jax import lax
from jax.sharding import PartitionSpec as P

HEAD_DIM = 64
WINDOW = 128
GRID_W = 64


def with_halo(cells, sides, width):
    for axis, dim in sides:
        count = lax.axis_size(axis)
        ends = count - 1
        head = lax.slice_in_dim(cells, 0, width, axis=dim)
        tail = lax.slice_in_dim(cells, cells.shape[dim] - width, cells.shape[dim], axis=dim)
        cells = jnp.concatenate(
            [
                lax.ppermute(tail, axis, [(i, (i + 1) % count) for i in range(ends)]),
                cells,
                lax.ppermute(head, axis, [((i + 1) % count, i) for i in range(ends)]),
            ],
            axis=dim,
        )
    return cells


def rotate(values, positions):
    quarter = 16
    inverse = 10000.0 ** (-jnp.arange(quarter, dtype=jnp.float32) / quarter)

    def turn(part, place):
        angle = place.astype(jnp.float32)[:, None] * inverse[None, :]
        cosine = jnp.cos(angle)[:, None, :]
        sine = jnp.sin(angle)[:, None, :]
        first, second = (part[..., :quarter], part[..., quarter:])
        return jnp.concatenate(
            [first * cosine - second * sine, second * cosine + first * sine], axis=-1
        )

    grid_row = positions // GRID_W
    grid_col = positions % GRID_W
    return jnp.concatenate(
        [turn(values[..., :32], grid_row), turn(values[..., 32:], grid_col)], axis=-1
    )


def share(weight, axis):
    parts = lax.axis_size("grp")
    size = weight.shape[axis] // parts
    part = lax.dynamic_slice_in_dim(weight, lax.axis_index("grp") * size, size, axis)
    return lax.all_gather(part, ("sp", "grp"), axis=axis, tiled=True)


def relay(blocks, axes, first_column):
    count, parts = lax.axis_size("sp"), lax.axis_size("grp")
    here, group = lax.axis_index("sp"), lax.axis_index("grp")

    def place(whole, value, axis, block, source, part):
        rows = block.shape[0]
        start = part * (rows // parts)
        at = (source * rows + start, 0)
        if axis == 1:
            columns = block.shape[1] * count
            at = (start, lax.rem(source * block.shape[1] + columns - first_column, columns))
        return lax.dynamic_update_slice(whole, value, at)

    wholes, right, left = [], [], []
    for block, axis in zip(blocks, axes):
        shape = list(block.shape)
        shape[axis] *= count
        wholes.append(place(jnp.zeros(shape, block.dtype), block, axis, block, here, 0))
        rows = block.shape[0] // parts
        part = lax.dynamic_slice_in_dim(block, group * rows, rows, 0)
        right.append([part])
        left.append([part])
    for step in range(1, count):
        source = jnp.where(here >= step, here - step, step)
        for index, (block, axis) in enumerate(zip(blocks, axes)):
            right[index].append(
                lax.ppermute(
                    right[index][-1], "sp", [(i, i + 1) for i in range(step - 1, count - 1)]
                )
            )
            left[index].append(
                lax.ppermute(left[index][-1], "sp", [(i + 1, i) for i in range(count - step)])
            )
            came = [left[index][step - i] for i in range(step)] + [right[index][step]]
            value = lax.select_n(jnp.minimum(here, step), *came)
            whole = place(wholes[index], value, axis, block, source, group)
            for shift in range(1, parts):
                other = lax.ppermute(value, "grp", [(i, (i + shift) % parts) for i in range(parts)])
                whole = place(whole, other, axis, block, source, (group - shift) % parts)
            wholes[index] = whole
    return wholes


def swap(value, bit):
    return lax.ppermute(value, "tp", [(i, i ^ bit) for i in range(lax.axis_size("tp"))])


def sum_columns(terms, bit):
    here = lax.axis_index("tp")
    while bit:
        half = terms.shape[1] // 2
        mine = jnp.where((here & bit) > 0, half, 0)
        theirs = lax.dynamic_slice_in_dim(terms, half - mine, half, 1).astype(jnp.bfloat16)
        own = lax.dynamic_slice_in_dim(terms, mine, half, 1)
        terms = own + swap(theirs, bit).astype(jnp.float32)
        bit //= 2
    return terms


def body(
    resid, queries, keys_values, sink, out_weight, norm_gain, gate_weight, up_weight, down_weight
):
    tok = queries.shape[0]
    heads_here = queries.shape[1] // HEAD_DIM
    kv_here = keys_values.shape[1]
    group = heads_here // kv_here
    cols = resid.shape[1]
    offset = lax.axis_index("sp") * tok
    total_tokens = tok * lax.axis_size("sp")
    positions = offset + jnp.arange(tok, dtype=jnp.int32)
    rotated_q = rotate(
        queries.astype(jnp.float32).reshape(tok, heads_here, HEAD_DIM), positions
    ).astype(jnp.bfloat16)
    padded = with_halo(keys_values, (("sp", 0),), WINDOW)
    ranks, members = lax.axis_size("sp"), lax.axis_size("tp")
    high = members // 2
    direct = ranks <= 8 and ranks % 2 == 0 and members >= 2 and members & (members - 1) == 0
    if direct:
        half_columns = resid.shape[1] * members // 2
        near = jnp.where((lax.axis_index("tp") & high) > 0, half_columns, 0)
        padded, gate_weight, up_weight, down_weight = lax.optimization_barrier(
            (padded, gate_weight, up_weight, down_weight)
        )
        whole_gate, whole_up, whole_down = relay(
            (gate_weight, up_weight, down_weight), (0, 0, 1), near
        )
    else:
        whole_gate, whole_up = share(gate_weight, 0), share(up_weight, 0)
        whole_down = share(down_weight, 1)
    whole_out = lax.all_gather(out_weight, "tp", axis=0, tiled=True)
    key_positions = offset - WINDOW + jnp.arange(tok + 2 * WINDOW, dtype=jnp.int32)
    rotated_k = rotate(padded[..., :HEAD_DIM].astype(jnp.float32), key_positions).astype(
        jnp.bfloat16
    )
    padded = jnp.concatenate([rotated_k, padded[..., HEAD_DIM:]], axis=-1)
    blocks = tok // WINDOW
    key_blocks = jnp.stack(
        [padded[index * WINDOW : index * WINDOW + 3 * WINDOW] for index in range(blocks)]
    )
    grouped = rotated_q.reshape(blocks, WINDOW, kv_here, group, HEAD_DIM)
    scores = jnp.einsum(
        "nqkgd,njkd->nkgqj", grouped, key_blocks[..., :HEAD_DIM], preferred_element_type=jnp.float32
    ) * HEAD_DIM ** (-0.5)
    block_start = offset + WINDOW * jnp.arange(blocks, dtype=jnp.int32)
    query_pos = block_start[:, None] + jnp.arange(WINDOW, dtype=jnp.int32)[None, :]
    key_pos = block_start[:, None] - WINDOW + jnp.arange(3 * WINDOW, dtype=jnp.int32)[None, :]
    valid = (
        (jnp.abs(query_pos[:, :, None] - key_pos[:, None, :]) <= WINDOW)
        & (key_pos[:, None, :] >= 0)
        & (key_pos[:, None, :] < total_tokens)
    )
    scores = jnp.where(valid[:, None, None], scores, jnp.float32(-1e30))
    sink_grid = sink.reshape(kv_here, group)[None, :, :, None]
    top = jnp.maximum(jnp.max(scores, axis=-1), sink_grid)
    expo = jnp.exp(scores - top[..., None])
    denom = jnp.sum(expo, axis=-1) + jnp.exp(sink_grid - top)
    probs = (expo / denom[..., None]).astype(jnp.bfloat16)
    attended = jnp.einsum(
        "nkgqj,njkd->nqkgd", probs, key_blocks[..., HEAD_DIM:], preferred_element_type=jnp.float32
    )
    attended = attended.astype(jnp.bfloat16).reshape(tok, heads_here * HEAD_DIM)
    attn_rows, resid_rows = (
        lax.all_to_all(attended, "tp", split_axis=0, concat_axis=1, tiled=True),
        lax.all_to_all(resid, "tp", split_axis=0, concat_axis=1, tiled=True),
    )
    stream_part = (
        resid_rows.astype(jnp.float32)
        + jnp.dot(attn_rows, whole_out, preferred_element_type=jnp.float32)
    ).astype(jnp.bfloat16)
    stream = lax.all_gather(stream_part, "tp", axis=0, tiled=True)
    stream_cols = lax.dynamic_slice_in_dim(stream, lax.axis_index("tp") * cols, cols, 1)
    widened = stream.astype(jnp.float32)
    normed = (
        widened * lax.rsqrt(jnp.mean(widened * widened, axis=-1, keepdims=True) + 1e-06) * norm_gain
    ).astype(jnp.bfloat16)
    gate = jnp.dot(normed, whole_gate, preferred_element_type=jnp.float32)
    up = jnp.dot(normed, whole_up, preferred_element_type=jnp.float32)
    hidden = (jax.nn.silu(gate) * up).astype(jnp.bfloat16)
    if direct:
        far_terms = jnp.dot(
            hidden, whole_down[:, half_columns:], preferred_element_type=jnp.float32
        )
        far_sum = swap(sum_columns(far_terms, high // 2).astype(jnp.bfloat16), high)
        near_terms = jnp.dot(
            hidden, whole_down[:, :half_columns], preferred_element_type=jnp.float32
        )
        near_sum = sum_columns(near_terms, high // 2)
        return (
            stream_cols.astype(jnp.float32) + (near_sum + far_sum.astype(jnp.float32))
        ).astype(jnp.bfloat16)
    terms = jnp.dot(
        hidden,
        whole_down,
        preferred_element_type=jnp.float32,
    )
    summed = lax.psum_scatter(
        terms.astype(jnp.bfloat16), "tp", scatter_dimension=1, tiled=True
    ).astype(jnp.float32)
    return (stream_cols.astype(jnp.float32) + summed).astype(jnp.bfloat16)


def solution(mesh):
    return jax.shard_map(
        body,
        mesh=mesh,
        in_specs=(
            P(("grp", "sp"), "tp"),
            P(("grp", "sp"), "tp"),
            P(("grp", "sp"), "tp", None),
            P("tp"),
            P("tp", None),
            P(),
            P("sp", "tp"),
            P("sp", "tp"),
            P("tp", "sp"),
        ),
        out_specs=P(("grp", "sp"), "tp"),
        check_vma=False,
    )
```

```python
import jax
import jax.numpy as jnp
from jax import lax
from jax.sharding import PartitionSpec as P

HEAD_DIM = 64
WINDOW = 128
GRID_W = 64


def with_halo(cells, sides, width):
    for axis, dim in sides:
        count = lax.axis_size(axis)
        ends = count - 1
        head = lax.slice_in_dim(cells, 0, width, axis=dim)
        tail = lax.slice_in_dim(cells, cells.shape[dim] - width, cells.shape[dim], axis=dim)
        cells = jnp.concatenate(
            [
                lax.ppermute(tail, axis, [(i, (i + 1) % count) for i in range(ends)]),
                cells,
                lax.ppermute(head, axis, [((i + 1) % count, i) for i in range(ends)]),
            ],
            axis=dim,
        )
    return cells


def rotate(values, positions):
    quarter = 16
    inverse = 10000.0 ** (-jnp.arange(quarter, dtype=jnp.float32) / quarter)

    def turn(part, place):
        angle = place.astype(jnp.float32)[:, None] * inverse[None, :]
        cosine = jnp.cos(angle)[:, None, :]
        sine = jnp.sin(angle)[:, None, :]
        first, second = (part[..., :quarter], part[..., quarter:])
        return jnp.concatenate(
            [first * cosine - second * sine, second * cosine + first * sine], axis=-1
        )

    grid_row = positions // GRID_W
    grid_col = positions % GRID_W
    return jnp.concatenate(
        [turn(values[..., :32], grid_row), turn(values[..., 32:], grid_col)], axis=-1
    )


def share(weight, axis):
    parts = lax.axis_size("grp")
    size = weight.shape[axis] // parts
    part = lax.dynamic_slice_in_dim(weight, lax.axis_index("grp") * size, size, axis)
    return lax.all_gather(part, ("sp", "grp"), axis=axis, tiled=True)


def relay(blocks, axes, first_column):
    count, parts = lax.axis_size("sp"), lax.axis_size("grp")
    here, group = lax.axis_index("sp"), lax.axis_index("grp")

    def place(whole, value, axis, block, source, part):
        rows = block.shape[0]
        start = part * (rows // parts)
        at = (source * rows + start, 0)
        if axis == 1:
            columns = block.shape[1] * count
            at = (start, lax.rem(source * block.shape[1] + columns - first_column, columns))
        if axis == 1 and part is not group:
            value = jnp.where(here < count, value, jnp.zeros_like(value))
        return lax.dynamic_update_slice(whole, value, at)

    wholes, right, left, late = [], [], [], []
    for block, axis in zip(blocks, axes):
        shape = list(block.shape)
        shape[axis] *= count
        wholes.append(place(jnp.zeros(shape, block.dtype), block, axis, block, here, 0))
        rows = block.shape[0] // parts
        part = lax.dynamic_slice_in_dim(block, group * rows, rows, 0)
        right.append([part])
        left.append([part])
    for step in range(1, count):
        source = jnp.where(here >= step, here - step, step)
        for index, (block, axis) in enumerate(zip(blocks, axes)):
            right[index].append(
                lax.ppermute(
                    right[index][-1], "sp", [(i, i + 1) for i in range(step - 1, count - 1)]
                )
            )
            left[index].append(
                lax.ppermute(left[index][-1], "sp", [(i + 1, i) for i in range(count - step)])
            )
            came = [left[index][step - i] for i in range(step)] + [right[index][step]]
            value = lax.select_n(jnp.minimum(here, step), *came)
            whole = place(wholes[index], value, axis, block, source, group)
            for shift in range(1, parts):
                other = lax.ppermute(value, "grp", [(i, (i + shift) % parts) for i in range(parts)])
                part = (group - shift) % parts
                if step == count - 1 and index == len(blocks) - 1:
                    late.append((other, axis, block, source, part))
                    continue
                whole = place(whole, other, axis, block, source, part)
            wholes[index] = whole

    def finish(whole):
        for piece in late:
            whole = place(whole, *piece)
        return whole

    return wholes, finish


def swap(value, bit):
    return lax.ppermute(value, "tp", [(i, i ^ bit) for i in range(lax.axis_size("tp"))])


def sum_columns(terms, bit):
    here = lax.axis_index("tp")
    while bit:
        half = terms.shape[1] // 2
        mine = jnp.where((here & bit) > 0, half, 0)
        theirs = lax.dynamic_slice_in_dim(terms, half - mine, half, 1).astype(jnp.bfloat16)
        own = lax.dynamic_slice_in_dim(terms, mine, half, 1)
        terms = own + swap(theirs, bit).astype(jnp.float32)
        bit //= 2
    return terms


def body(
    resid, queries, keys_values, sink, out_weight, norm_gain, gate_weight, up_weight, down_weight
):
    tok = queries.shape[0]
    heads_here = queries.shape[1] // HEAD_DIM
    kv_here = keys_values.shape[1]
    group = heads_here // kv_here
    cols = resid.shape[1]
    offset = lax.axis_index("sp") * tok
    total_tokens = tok * lax.axis_size("sp")
    positions = offset + jnp.arange(tok, dtype=jnp.int32)
    rotated_q = rotate(
        queries.astype(jnp.float32).reshape(tok, heads_here, HEAD_DIM), positions
    ).astype(jnp.bfloat16)
    padded = with_halo(keys_values, (("sp", 0),), WINDOW)
    ranks, members = lax.axis_size("sp"), lax.axis_size("tp")
    high = members // 2
    direct = ranks <= 8 and ranks % 2 == 0 and members >= 2 and members & (members - 1) == 0
    if direct:
        half_columns = resid.shape[1] * members // 2
        near = jnp.where((lax.axis_index("tp") & high) > 0, half_columns, 0)
        padded, gate_weight, up_weight, down_weight = lax.optimization_barrier(
            (padded, gate_weight, up_weight, down_weight)
        )
        both = jnp.concatenate([gate_weight, up_weight], axis=1)
        (whole_both, whole_down), late = relay((both, down_weight), (0, 1), near)
    else:
        whole_both = jnp.concatenate([share(gate_weight, 0), share(up_weight, 0)], axis=1)
        whole_down = share(down_weight, 1)
    whole_out = lax.all_gather(out_weight, "tp", axis=0, tiled=True)
    key_positions = offset - WINDOW + jnp.arange(tok + 2 * WINDOW, dtype=jnp.int32)
    rotated_k = rotate(padded[..., :HEAD_DIM].astype(jnp.float32), key_positions).astype(
        jnp.bfloat16
    )
    padded = jnp.concatenate([rotated_k, padded[..., HEAD_DIM:]], axis=-1)
    blocks = tok // WINDOW
    key_blocks = jnp.stack(
        [padded[index * WINDOW : index * WINDOW + 3 * WINDOW] for index in range(blocks)]
    )
    grouped = rotated_q.reshape(blocks, WINDOW, kv_here, group, HEAD_DIM)
    scores = jnp.einsum(
        "nqkgd,njkd->nkgqj", grouped, key_blocks[..., :HEAD_DIM], preferred_element_type=jnp.float32
    ) * HEAD_DIM ** (-0.5)
    block_start = offset + WINDOW * jnp.arange(blocks, dtype=jnp.int32)
    query_pos = block_start[:, None] + jnp.arange(WINDOW, dtype=jnp.int32)[None, :]
    key_pos = block_start[:, None] - WINDOW + jnp.arange(3 * WINDOW, dtype=jnp.int32)[None, :]
    valid = (
        (jnp.abs(query_pos[:, :, None] - key_pos[:, None, :]) <= WINDOW)
        & (key_pos[:, None, :] >= 0)
        & (key_pos[:, None, :] < total_tokens)
    )
    scores = jnp.where(valid[:, None, None], scores, jnp.float32(-1e30))
    sink_grid = sink.reshape(kv_here, group)[None, :, :, None]
    top = jnp.maximum(jnp.max(scores, axis=-1), sink_grid)
    expo = jnp.exp(scores - top[..., None])
    denom = jnp.sum(expo, axis=-1) + jnp.exp(sink_grid - top)
    probs = (expo / denom[..., None]).astype(jnp.bfloat16)
    attended = jnp.einsum(
        "nkgqj,njkd->nqkgd", probs, key_blocks[..., HEAD_DIM:], preferred_element_type=jnp.float32
    )
    attended = attended.astype(jnp.bfloat16).reshape(tok, heads_here * HEAD_DIM)
    attn_rows, resid_rows = (
        lax.all_to_all(attended, "tp", split_axis=0, concat_axis=1, tiled=True),
        lax.all_to_all(resid, "tp", split_axis=0, concat_axis=1, tiled=True),
    )
    stream_part = (
        resid_rows.astype(jnp.float32)
        + jnp.dot(attn_rows, whole_out, preferred_element_type=jnp.float32)
    ).astype(jnp.bfloat16)
    stream = lax.all_gather(stream_part, "tp", axis=0, tiled=True)
    stream_cols = lax.dynamic_slice_in_dim(stream, lax.axis_index("tp") * cols, cols, 1)
    widened = stream.astype(jnp.float32)
    normed = (
        widened * lax.rsqrt(jnp.mean(widened * widened, axis=-1, keepdims=True) + 1e-06) * norm_gain
    ).astype(jnp.bfloat16)
    gate_up = jnp.dot(normed, whole_both, preferred_element_type=jnp.float32)
    gate, up = jnp.split(gate_up, 2, axis=1)
    hidden = (jax.nn.silu(gate) * up).astype(jnp.bfloat16)
    if direct:
        hidden, whole_down = lax.optimization_barrier((hidden, whole_down))
        whole_down = late(whole_down)
        far_terms = jnp.dot(
            hidden, whole_down[:, half_columns:], preferred_element_type=jnp.float32
        )
        far_sum = swap(sum_columns(far_terms, high // 2).astype(jnp.bfloat16), high)
        near_terms = jnp.dot(
            hidden, whole_down[:, :half_columns], preferred_element_type=jnp.float32
        )
        near_sum = sum_columns(near_terms, high // 2)
        return (
            stream_cols.astype(jnp.float32) + (near_sum + far_sum.astype(jnp.float32))
        ).astype(jnp.bfloat16)
    terms = jnp.dot(
        hidden,
        whole_down,
        preferred_element_type=jnp.float32,
    )
    summed = lax.psum_scatter(
        terms.astype(jnp.bfloat16), "tp", scatter_dimension=1, tiled=True
    ).astype(jnp.float32)
    return (stream_cols.astype(jnp.float32) + summed).astype(jnp.bfloat16)


def solution(mesh):
    return jax.shard_map(
        body,
        mesh=mesh,
        in_specs=(
            P(("grp", "sp"), "tp"),
            P(("grp", "sp"), "tp"),
            P(("grp", "sp"), "tp", None),
            P("tp"),
            P("tp", None),
            P(),
            P("sp", "tp"),
            P("sp", "tp"),
            P("tp", "sp"),
        ),
        out_specs=P(("grp", "sp"), "tp"),
        check_vma=False,
    )
```
